32 devices in a mesh: kv: 8 (over z, y), tp: 4 (over x, core).
Axes of the slice: x: 2, y: 2, z: 4, core: 2. Of those that a mesh axis runs over, the one named last changes fastest.
Arguments:
- tokens: bfloat16 [128, 4096], P(None, 'kv'), may hold values from -152 to 152, as said below
- norm_gain: float32 [4096], P('kv'), may hold values from 0.1 to 1.9
- w_query: bfloat16 [4096, 2048], P('kv', 'tp'), may hold values from -0.09375 to 0.09375
- w_key: bfloat16 [4096, 2048], P('kv', 'tp'), may hold values from -0.375 to 0.375
- w_value: bfloat16 [4096, 2048], P('kv', 'tp'), may hold values from -0.09375 to 0.09375
- lambdas: float32 [16], P('tp'), may hold values from 0.3 to 0.8
- head_gain: float32 [128], replicated, may hold values from 0.1 to 1.9
- w_out: bfloat16 [2048, 4096], P('tp', 'kv'), may hold values from -0.125 to 0.125
- cache_keys: bfloat16 [8, 4096, 16, 128], P(None, 'kv', 'tp'), may hold values from -370 to 370
- cache_values: bfloat16 [8, 4096, 16, 128], P(None, 'kv', 'tp'), may hold values from -6 to 6
- lengths: int32 [8], replicated, may hold values from 2560 to 4074
- accepted: int32 [8], replicated, may hold values from 0 to 6
- parents: int32 [8, 16], replicated, may hold values from -1 to 14, as said below
Outputs:
- layer_out: bfloat16 [128, 4096], P('tp', 'kv')
- keys_out: bfloat16 [8, 4096, 16, 128], P(None, 'kv', 'tp')
- values_out: bfloat16 [8, 4096, 16, 128], P(None, 'kv', 'tp')
The draws below stay inside these ranges and needn't reach their ends.
Inputs may be any that keep to these rules, and one draw needn't show every extreme that they name: `tokens`: columns of features have scales that differ; rows too. The proposals of the last step that were kept already stand right after the first lengths positions; the next 16 positions receive this step's proposals. `parents`: proposal 0 of every sequence has parent -1; every other proposal's parent is an earlier proposal of the same sequence, and the last proposal's parent is the one right before it.
All inputs are finite; a program needn't handle non-finite values.
Results may differ from the reference program's by a relative error of at most 0.015.
The reference program's roundings to bfloat16 on the way count: a program that leaves them out, or rounds other values in their place, can miss the bound.
Values may be sent and summed in bfloat16 or wider, within the bound.
A program may use at most 64 MiB of HBM per device.

```python
import jax
import jax.numpy as jnp
from jax import lax

D = 4096
HEADS = 16
HEAD = 64
KDIM = 128
GROUP_HEADS = 4
SEQS = 8
POS_DEV = 512
PROP = 16
ACC_MOST = 6
CACHE = 4096
TOKENS = 128
N_KV = 8
N_TP = 4


def draw_tokens(key, part):
    key_base, key_rough, key_rows = jax.random.split(key, 3)
    normals = jax.random.truncated_normal(key_base, -4.0, 4.0, (TOKENS, D), jnp.float32)
    fraction = jnp.arange(D, dtype=jnp.float32) / (D - 1)
    roughness = jax.random.uniform(key_rough, (D,), jnp.float32, 0.7, 1.4)
    columns = jnp.exp(jnp.log(3.0) * fraction) * roughness
    row_scales = jnp.exp(jax.random.uniform(key_rows, (TOKENS, 1), jnp.float32, jnp.log(0.5), jnp.log(2.0)))
    return (normals * columns[None, :] * row_scales).astype(jnp.bfloat16)


def draw_cache_keys(key, part):
    key_base = jax.random.fold_in(key, 0)
    array_shape = (SEQS, CACHE, HEADS, KDIM)
    drawn = 1.75 * jax.random.truncated_normal(key_base, -6.0, 6.0, array_shape, jnp.float32)
    return drawn.astype(jnp.bfloat16)


def draw_parents(key, part):
    drawn_ints = jax.random.randint(key, (SEQS, PROP), 0, 1 << 20)
    members = jnp.arange(PROP, dtype=jnp.int32)[None, :]
    chosen = drawn_ints % jnp.maximum(members, 1)
    chosen = jnp.where(members == PROP - 1, PROP - 2, chosen)
    return jnp.where(members == 0, -1, chosen).astype(jnp.int32)


def plant(array, rng, low, high):
    spot = [jax.random.randint(jax.random.fold_in(rng, axis), (), 0, length) for axis, length in enumerate(array.shape)]
    main_axis = array.shape.index(max(array.shape))
    next_to = spot[:main_axis] + [(spot[main_axis] + 1) % array.shape[main_axis]] + spot[main_axis + 1:]
    return array.at[tuple(spot)].set(low).at[tuple(next_to)].set(high)


def level_of(stream_key, shape, shards, low, high):
    gain, own = 1.0, jax.random.fold_in(stream_key, 6)
    for dim, parts in shards:
        draws = jnp.exp(jax.random.uniform(jax.random.fold_in(own, dim), (parts,), jnp.float32, low / len(shards), high / len(shards)))
        gain = gain * jnp.repeat(draws, shape[dim] // parts).reshape([-1 if axis == dim else 1 for axis in range(len(shape))])
    return gain


def centred(own_key, shape, deviation, limit, shards=(), kind=jnp.bfloat16):
    entries = jax.random.normal(own_key, shape, jnp.float32) * deviation
    if len(shards) > 0:
        entries = level_of(own_key, shape, shards, -0.22, 0.18) * entries
    return jnp.clip(entries, min=-limit, max=limit).astype(kind)


def setup_inputs(seed: int = 0) -> dict:
    seeds = jax.random.split(jax.random.key(seed), 14)
    tokens = draw_tokens(jax.random.fold_in(seeds[13], 71), 0)
    norm_gain = jnp.clip(1.0 + 0.18 * jax.random.normal(seeds[1], (D,), jnp.float32), 0.1, 1.9)
    w_query = centred(seeds[2], (D, HEADS * KDIM), D ** -0.5, 0.09375, ((0, 8), (1, 4)))
    w_key = centred(seeds[3], (D, HEADS * KDIM), (4.0 * D ** -0.5), 0.375, ((0, 8), (1, 4)))
    w_value = centred(seeds[4], (D, HEADS * KDIM), D ** -0.5, 0.09375, ((0, 8), (1, 4)))
    lambdas = jnp.clip(0.3 + 0.5 * jax.random.uniform(seeds[5], (HEADS,), jnp.float32) ** level_of(seeds[5], (HEADS,), ((0, 4),), -0.2, 0.2), 0.3, 0.8)
    head_gain = jnp.clip(1.0 + 0.18 * jax.random.normal(seeds[6], (KDIM,), jnp.float32), 0.1, 1.9)
    w_out = centred(seeds[7], (HEADS * KDIM, D), (HEADS * KDIM) ** -0.5, 0.125, ((0, 4), (1, 8)))
    cache_keys = draw_cache_keys(jax.random.fold_in(seeds[13], 71), 0)
    cache_values = centred(seeds[9], (SEQS, CACHE, HEADS, KDIM), 1.0, 6.0, ((1, 8), (2, 4)))
    lengths = plant(jax.random.randint(seeds[10], (SEQS,), CACHE // 2 + POS_DEV, CACHE - PROP - ACC_MOST + 1), jax.random.fold_in(seeds[10], 1), CACHE // 2 + POS_DEV, CACHE - PROP - ACC_MOST).astype(jnp.int32)
    accepted = plant(jax.random.randint(seeds[11], (SEQS,), 0, ACC_MOST + 1), jax.random.fold_in(seeds[11], 1), 0, ACC_MOST).astype(jnp.int32)
    parents = draw_parents(jax.random.fold_in(seeds[13], 71), 0)
    return dict(tokens=tokens, norm_gain=norm_gain, w_query=w_query, w_key=w_key, w_value=w_value, lambdas=lambdas, head_gain=head_gain, w_out=w_out, cache_keys=cache_keys, cache_values=cache_values, lengths=lengths, accepted=accepted, parents=parents)


eps_row = 1e-06
eps_head = 1e-05
masked = -1e+30

def ancestry(parents):
    members = parents.shape[0]
    indices = jnp.arange(members, dtype=jnp.int32)
    reachable = (parents[:, None] == indices[None, :]).astype(jnp.float32) + jnp.eye(members, dtype=jnp.float32)
    for repeat in range(max(1, (members - 1).bit_length())):
        reachable = jnp.minimum(jnp.dot(reachable, reachable, precision=lax.Precision.HIGHEST), 1.0)
    return reachable

def reference(tokens, norm_gain, w_query, w_key, w_value, lambdas, head_gain, w_out, cache_keys, cache_values, lengths, accepted, parents):
    widened = tokens.astype(jnp.float32)
    row_scale = lax.rsqrt(lax.optimization_barrier(jnp.mean(widened * widened, axis=1, keepdims=True)) + eps_row)
    scaled = (widened * norm_gain[None, :]).astype(jnp.bfloat16)

    def project(weight):
        summed_rows = jnp.dot(scaled, weight, preferred_element_type=jnp.float32)
        return (row_scale * summed_rows).astype(jnp.bfloat16).reshape(SEQS, PROP, HEADS, KDIM)
    queries = project(w_query)
    new_keys = project(w_key)
    new_values = project(w_value)
    limits = (lengths + accepted).astype(jnp.int32)
    score_scale = HEAD ** (-0.5)

    def one_sequence(inputs):
        query_rows, key_new, value_new, key_old, value_old, valid_len, parent = inputs
        query_pairs = query_rows.reshape(PROP, HEADS, 2, HEAD).astype(jnp.float32)
        new_pairs = key_new.reshape(PROP, HEADS, 2, HEAD).astype(jnp.float32)
        key_pairs = key_old.reshape(N_KV, POS_DEV, HEADS, 2, HEAD).astype(jnp.float32)
        value_blocks = value_old.reshape(N_KV, POS_DEV, HEADS, KDIM).astype(jnp.float32)
        positions = jnp.arange(CACHE, dtype=jnp.int32).reshape(N_KV, POS_DEV)
        usable = (positions < valid_len)[None, None, None]
        scores = jnp.einsum('jhmd,nphmd->jhmnp', query_pairs, key_pairs) * score_scale
        scores = jnp.where(usable, scores, masked)
        maxima = lax.optimization_barrier(jnp.max(scores, axis=4))
        weights = jnp.where(usable, jnp.exp(scores - maxima[..., None]), 0.0)
        totals = lax.optimization_barrier(jnp.sum(weights, axis=4))
        rounded = lax.optimization_barrier(weights.astype(jnp.bfloat16)).astype(jnp.float32)
        summed = jnp.einsum('jhmnp,nphd->jhmnd', rounded, value_blocks)
        in_tree = (ancestry(parent) > 0.5)[:, None, None, :]
        tree_scores = jnp.einsum('jhmd,ihmd->jhmi', query_pairs, new_pairs) * score_scale
        tree_scores = jnp.where(in_tree, tree_scores, masked)
        tree_max = lax.optimization_barrier(jnp.max(tree_scores, axis=3))
        tree_weights = jnp.where(in_tree, jnp.exp(tree_scores - tree_max[..., None]), 0.0)
        tree_totals = lax.optimization_barrier(jnp.sum(tree_weights, axis=3))
        tree_rounded = lax.optimization_barrier(tree_weights.astype(jnp.bfloat16)).astype(jnp.float32)
        tree_summed = jnp.einsum('jhmi,ihd->jhmd', tree_rounded, value_new.astype(jnp.float32))
        highest = jnp.maximum(lax.optimization_barrier(jnp.max(maxima, axis=3)), tree_max)
        factors = jnp.exp(maxima - highest[..., None])
        tree_factor = jnp.exp(tree_max - highest)
        denominator = lax.optimization_barrier(jnp.sum(totals * factors, axis=3)) + tree_totals * tree_factor
        numerator = lax.optimization_barrier(jnp.sum(summed * factors[..., None], axis=3)) + tree_summed * tree_factor[..., None]
        attended = numerator / denominator[..., None]
        return attended[:, :, 0] - lambdas[None, :, None] * attended[:, :, 1]
    heads_out = lax.map(one_sequence, (queries, new_keys, new_values, cache_keys, cache_values, limits, parents))
    inverse_rms = lax.rsqrt(lax.optimization_barrier(jnp.mean(heads_out * heads_out, axis=3, keepdims=True)) + eps_head)
    normed = (heads_out * inverse_rms * head_gain).astype(jnp.bfloat16)
    grouped = normed.reshape(TOKENS, N_TP, GROUP_HEADS * KDIM).astype(jnp.float32)
    w_groups = w_out.reshape(N_TP, GROUP_HEADS * KDIM, D).astype(jnp.float32)
    partial_value = jnp.einsum('tgc,gcd->gtd', grouped, w_groups).astype(jnp.bfloat16)
    layer_out = lax.optimization_barrier(jnp.sum(partial_value.astype(jnp.float32), axis=0)).astype(jnp.bfloat16)

    def place(sequence, caches):
        keys_now, values_now = caches
        seq_index = jnp.asarray(sequence).astype(jnp.int32)
        first_slot = lax.dynamic_index_in_dim(limits, seq_index, keepdims=False).astype(jnp.int32)
        fresh_keys = lax.dynamic_index_in_dim(new_keys, seq_index, keepdims=True)
        fresh_values = lax.dynamic_index_in_dim(new_values, seq_index, keepdims=True)
        anchor = jnp.zeros((), jnp.int32)
        start_at = (seq_index, first_slot, anchor, anchor)
        return (lax.dynamic_update_slice(keys_now, fresh_keys, start_at), lax.dynamic_update_slice(values_now, fresh_values, start_at))
    keys_out, values_out = lax.fori_loop(0, SEQS, place, (cache_keys, cache_values))
    return (layer_out, keys_out, values_out)
```

```python
import functools

import jax
import jax.numpy as jnp
from jax import lax
from jax.experimental import pallas as pl
from jax.experimental.pallas import tpu as pltpu
from jax.sharding import PartitionSpec as P

KDIM = 128
HEAD = 64
PROP = 16

eps_row = 1e-06
eps_head = 1e-05
masked = -1e30
floor_max = -1e29

MESH = pl.DeviceIdType.MESH
VMEM = pl.BlockSpec(memory_space=pltpu.VMEM)
ANY = pl.BlockSpec(memory_space=pl.ANY)
SMEM = pl.BlockSpec(memory_space=pltpu.SMEM)
NT = (((1,), (1,)), ((), ()))
f32 = jnp.float32
bf16 = jnp.bfloat16


def iota(shape, dim):
    return lax.broadcasted_iota(jnp.int32, shape, dim)


def remote(src, dst, send, recv, **where):
    return pltpu.make_async_remote_copy(
        src_ref=src, dst_ref=dst, send_sem=send, recv_sem=recv, device_id=where, device_id_type=MESH
    )


def arrived(ref, send, recv, **where):
    remote(ref, ref, send, recv, **where).wait_recv()


def pair_rows(queries, heads):
    lane = iota((PROP, KDIM), 1)
    columns = [queries[:, h * KDIM : (h + 1) * KDIM].astype(f32) * (HEAD ** (-0.5)) for h in range(heads)]
    rows = [jnp.where(lane < HEAD, c, 0.0) for c in columns]
    rows += [jnp.where(lane >= HEAD, c, 0.0) for c in columns]
    return jnp.concatenate(rows, axis=0).astype(bf16)


def head_rows(array, heads):
    return jnp.concatenate([array[:, h * KDIM : (h + 1) * KDIM] for h in range(heads)], axis=0)


def stat_rows(maxima, totals):
    rows = maxima.shape[0]
    lane = iota((rows, KDIM), 1)
    wide = jnp.where(lane == 0, maxima, jnp.where(lane == 1, totals, 0.0))
    if rows < KDIM:
        wide = jnp.concatenate([wide, jnp.ones((KDIM - rows, KDIM), f32)], axis=0)
    return wide.T[:8, :]


def tree_part(own_queries, fresh, parent_row, heads):
    columns = heads * KDIM
    queries = pair_rows(own_queries, heads)
    keys = head_rows(fresh[:, :columns], heads)
    values = head_rows(fresh[:, columns:], heads)
    below = iota((PROP, PROP), 0)
    reach = jnp.logical_or(parent_row == below, below == iota((PROP, PROP), 1)).astype(f32)
    for repeat in range(max(1, (PROP - 1).bit_length())):
        narrow = reach.astype(bf16)
        reach = jnp.minimum(jnp.dot(narrow, narrow, preferred_element_type=f32), 1.0)
    rows, cols = 2 * heads * PROP, heads * PROP
    pick = (lax.rem(iota((rows, PROP), 0), PROP) == iota((rows, PROP), 1)).astype(bf16)
    spread = (lax.rem(iota((PROP, cols), 1), PROP) == iota((PROP, cols), 0)).astype(bf16)
    picked = lax.dot_general(pick, reach.astype(bf16), NT, preferred_element_type=f32)
    related = jnp.dot(picked.astype(bf16), spread, preferred_element_type=f32) > 0.5
    same = lax.rem(iota((rows, cols), 0) // PROP, heads) == iota((rows, cols), 1) // PROP
    s = lax.dot_general(queries, keys, NT, preferred_element_type=f32)
    allowed = jnp.logical_and(related, same)
    s = jnp.where(allowed, s, masked)
    top = jnp.max(s, axis=1, keepdims=True)
    w = jnp.where(allowed, jnp.exp(s - top), 0.0)
    total = jnp.sum(w, axis=1, keepdims=True)
    return top, total, jnp.dot(w.astype(bf16), values, preferred_element_type=f32)


def layer_kernel(n, n_tp, x_ref, gain_ref, wq_hbm, wk_hbm, wv_hbm, lam_ref, head_gain_ref, wo_hbm, ck_hbm, cv_hbm, len_ref, acc_ref, parents_ref,
                 out_ref, fresh_ref, *scratch):
    (w_in, wo, keys, values, part, send_q, send_k, send_v, recv_q, recv_k, recv_v, queries, scale, head_bias,
     scores_a, scores_b, weights_a, weights_b, sums, stats, got, got_stats, shares, normed, parts, got_parts,
     w_sem, c_sem, rs_s, rs_r, q_s, q_r, f_s, f_r, x_s, x_r, g_s, g_r, p_s, p_r) = scratch
    me = lax.axis_index("kv")
    tp = lax.axis_index("tp")
    sequences, rows_block, _ = ck_hbm.shape
    features, columns = wq_hbm.shape
    heads = columns // KDIM
    rows = 2 * heads * PROP
    positions = rows_block // heads
    group = n // sequences
    mine = me // group
    own = lax.rem(me, group) == 0
    barrier = pltpu.get_barrier_semaphore()
    for o in range(1, n):
        pl.semaphore_signal(barrier, inc=1, device_id={"kv": lax.rem(me + o, n)}, device_id_type=MESH)
    for o in range(1, n_tp):
        pl.semaphore_signal(barrier, inc=1, device_id={"tp": lax.rem(tp + o, n_tp)}, device_id_type=MESH)

    def when_own(run):
        if group > 1:
            pl.when(own)(run)
        else:
            run()

    def when_foreign(run):
        if group > 1:
            pl.when(jnp.logical_not(own))(run)

    def turn(o):
        return lax.rem(mine + o, sequences)

    local = [pltpu.make_async_copy(h, w_in.at[k], w_sem.at[k]) for k, h in enumerate((wq_hbm, wk_hbm, wv_hbm))]
    for copy in local:
        copy.start()

    def cached(k, b):
        return pltpu.make_async_copy((ck_hbm, cv_hbm)[k].at[b], (keys, values)[k].at[b], c_sem.at[k, b])

    for o in range(sequences):
        for k in range(2):
            cached(k, turn(o)).start()
    w_out_copy = pltpu.make_async_copy(wo_hbm, wo, w_sem.at[3])
    w_out_copy.start()

    wide = x_ref[...].astype(f32)
    scaled = (wide * gain_ref[...]).astype(bf16)
    squares = wide * wide
    folded = squares[:, :KDIM]
    for c in range(KDIM, features, KDIM):
        folded = folded + squares[:, c : c + KDIM]
    first_columns = columns + KDIM
    starts = (0, first_columns, first_columns + columns)
    sends, recvs = (send_q, send_k, send_v), (recv_q, recv_k, recv_v)
    part[:, :, columns:first_columns] = folded.reshape(sequences, PROP, KDIM)
    send_q[:, :, columns:] = folded.astype(bf16).reshape(sequences, PROP, KDIM)

    def project(k):
        local[k].wait()
        product = jnp.dot(scaled, w_in[k], preferred_element_type=f32)
        part[:, :, starts[k] : starts[k] + columns] = product.reshape(sequences, PROP, columns)
        sends[k][:, :, :columns] = product.astype(bf16).reshape(sequences, PROP, columns)

    def scatter(k, o):
        b = turn(o)
        return remote(sends[k].at[b], recvs[k].at[me], rs_s.at[k, b], rs_r.at[k, me], kv=b * group)

    def scatter_all(k):
        for o in range(1, sequences):
            scatter(k, o).start()
        when_foreign(lambda: scatter(k, 0).start())

    def summed(k, width):
        total = part[mine, :, starts[k] : starts[k] + width]
        for o in range(1, n):
            source = lax.rem(me + n - o, n)
            arrived(recvs[k].at[source], rs_s.at[k, 0], rs_r.at[k, source], kv=source)
            total = total + recvs[k][source].astype(f32)
        return total

    def spread(ref, send, recv):
        return [remote(ref.at[mine], ref.at[mine], send.at[o], recv.at[mine], kv=lax.rem(me + o, n)) for o in range(1, n)]

    def gathered(ref, send, recv, b):
        arrived(ref.at[b], send.at[0], recv.at[b], kv=b * group)

    project(0)
    pl.semaphore_wait(barrier, n - 1 + n_tp - 1)
    scatter_all(0)
    project(1)
    scatter_all(1)
    project(2)

    lane_head = lax.rem(iota((8, rows_block), 1), heads)
    for h in range(heads):
        head_bias[h] = jnp.where(lane_head == h, 0.0, masked)

    def finish_queries():
        total = summed(0, first_columns)
        mean = jnp.sum(total[:, columns:], axis=1, keepdims=True) / (features * n)
        inverse = lax.rsqrt(mean + eps_row)
        scale[...] = jnp.broadcast_to(inverse, scale.shape)
        queries[mine] = (inverse * total[:, :columns]).astype(bf16)
        for copy in spread(queries, q_s, q_r):
            copy.start()

    when_own(finish_queries)
    scatter_all(2)

    column = iota((8, rows_block), 1)

    def exchange(b):
        return (
            remote(sums.at[b], got.at[me], x_s.at[0, b], x_r.at[0, me], kv=b * group),
            remote(stats.at[b], got_stats.at[me], x_s.at[1, b], x_r.at[1, me], kv=b * group),
        )

    def attend(i, carry):
        two = (2 * i, 2 * i + 1)
        places = [turn(o) for o in two]
        for o, b in zip(two, places):
            for k in range(2):
                cached(k, b).wait()

            @pl.when(jnp.logical_or(o > 0, jnp.logical_not(own)))
            def _():
                gathered(queries, q_s, q_r, b)
        scored, weighed = (scores_a, scores_b), (weights_a, weights_b)
        for b, s_ref in zip(places, scored):
            s_ref[...] = lax.dot_general(pair_rows(queries[b], heads), keys[b], NT, preferred_element_type=f32)
        for b, s_ref, w_ref in zip(places, scored, weighed):
            limit = len_ref[b] + acc_ref[b] - me * positions
            beyond = jnp.where(column < limit * heads, 0.0, masked)
            maxima, totals = [None] * (2 * heads), [None] * (2 * heads)
            for h in range(heads):
                bias = head_bias[h] + beyond
                bias = jnp.concatenate([bias, bias], axis=0)
                for m in range(2):
                    r = m * heads + h
                    s = s_ref[r * PROP : (r + 1) * PROP, :] + bias
                    top = jnp.maximum(jnp.max(s, axis=1, keepdims=True), floor_max)
                    w = jnp.exp(s - top)
                    w_ref[r * PROP : (r + 1) * PROP, :] = w.astype(bf16)
                    maxima[r] = top
                    totals[r] = jnp.sum(w, axis=1, keepdims=True)
            sums[b] = jnp.dot(w_ref[...], values[b], preferred_element_type=f32).astype(bf16)
            stats[b] = stat_rows(jnp.concatenate(maxima, axis=0), jnp.concatenate(totals, axis=0))
        for o, b in zip(two, places):
            @pl.when(jnp.logical_or(o > 0, jnp.logical_not(own)))
            def _():
                for copy in exchange(b):
                    copy.start()
        return carry

    lax.fori_loop(0, sequences // 2, attend, 0)

    def finish_fresh():
        for k in (1, 2):
            fresh_ref[mine, :, (k - 1) * columns : k * columns] = (scale[:, :1] * summed(k, columns)).astype(bf16)
        for copy in spread(fresh_ref, f_s, f_r):
            copy.start()

    when_own(finish_fresh)

    def finish():
        top, total, tree_sums = tree_part(queries[mine], fresh_ref[mine], parents_ref[pl.ds(mine, 1), :], heads)
        tree = stat_rows(top, total)
        got_stats[me] = stats[mine]
        for o in range(1, n):
            source = lax.rem(me + n - o, n)
            arrived(got_stats.at[source], x_s.at[1, 0], x_r.at[1, source], kv=source)
        highest = tree[0:1]
        for s in range(n):
            highest = jnp.maximum(highest, got_stats[s, 0:1, :])
        tree_share = jnp.exp(tree[0:1] - highest)
        bottom = tree_share * tree[1:2]
        factors = []
        for s in range(n):
            factors.append(jnp.exp(got_stats[s, 0:1, :] - highest))
            bottom = bottom + factors[s] * got_stats[s, 1:2, :]
        shares[...] = jnp.zeros_like(shares)
        for s in range(n):
            shares[s : s + 1, :] = factors[s] / bottom
        shares[n : n + 1, :] = tree_share / bottom
        turned = shares[...].T[:rows]
        attended = turned[:, n : n + 1] * tree_sums
        got[me] = sums[mine]
        for o in range(1, n):
            source = lax.rem(me + n - o, n)
            arrived(got.at[source], x_s.at[0, 0], x_r.at[0, source], kv=source)
        for s in range(n):
            attended = attended + turned[:, s : s + 1] * got[s].astype(f32)
        half = rows // 2
        for h in range(heads):
            first = attended[h * PROP : (h + 1) * PROP]
            second = attended[half + h * PROP : half + (h + 1) * PROP]
            blended = first - lam_ref[h] * second
            mean = jnp.mean(blended * blended, axis=1, keepdims=True)
            value = (blended * lax.rsqrt(mean + eps_head) * head_gain_ref[...]).astype(bf16)
            normed[mine, :, h * KDIM : (h + 1) * KDIM] = value
        for copy in spread(normed, g_s, g_r):
            copy.start()

    when_own(finish)
    w_out_copy.wait()
    for o in range(1, sequences):
        gathered(normed, g_s, g_r, turn(o))
    when_foreign(lambda: gathered(normed, g_s, g_r, mine))
    everything = normed[...].reshape(sequences * PROP, columns)
    product = jnp.dot(everything, wo[...], preferred_element_type=f32)
    parts[...] = product.astype(bf16).reshape(parts.shape)

    def partial(o):
        to = lax.rem(tp + o, n_tp)
        return remote(parts.at[to], got_parts.at[tp], p_s.at[o], p_r.at[tp], tp=to)

    for o in range(1, n_tp):
        partial(o).start()
    for o in range(1, sequences):
        gathered(fresh_ref, f_s, f_r, turn(o))
    when_foreign(lambda: gathered(fresh_ref, f_s, f_r, mine))

    def sent(b):
        for copy in exchange(b):
            copy.wait_send()

    for o in range(1, sequences):
        for k in range(3):
            scatter(k, o).wait_send()
        sent(turn(o))

    def foreign_drain():
        for k in range(3):
            scatter(k, 0).wait_send()
        sent(mine)

    when_foreign(foreign_drain)

    def drain():
        for copy in spread(queries, q_s, q_r) + spread(fresh_ref, f_s, f_r) + spread(normed, g_s, g_r):
            copy.wait_send()

    when_own(drain)
    total = parts[tp].astype(f32)
    for o in range(1, n_tp):
        source = lax.rem(tp + n_tp - o, n_tp)
        arrived(got_parts.at[source], p_s.at[0], p_r.at[source], tp=source)
        total = total + got_parts[source].astype(f32)
    out_ref[...] = total.astype(bf16)
    for o in range(1, n_tp):
        partial(o).wait_send()


def place_kernel(heads, len_ref, acc_ref, fresh_ref, k_hbm, v_hbm, ko_hbm, vo_hbm, keys, values, in_sem, out_sem):
    sequences, rows_block, _ = k_hbm.shape
    columns = heads * KDIM
    positions = rows_block // heads
    start = lax.axis_index("kv") * positions
    sources, held, targets = (k_hbm, v_hbm), (keys, values), (ko_hbm, vo_hbm)

    def load(b, k):
        return pltpu.make_async_copy(sources[k].at[b], held[k].at[b], in_sem.at[k, b])

    def store(b, k):
        return pltpu.make_async_copy(held[k].at[b], targets[k].at[b], out_sem.at[k, b])

    every = [(b, k) for b in range(sequences) for k in range(2)]
    for b, k in every:
        load(b, k).start()
    window = (heads + 1) * PROP
    cols = heads * PROP
    row0 = iota((window, cols), 0)
    col = iota((window, cols), 1)
    wanted = lax.rem(col, PROP) * heads + col // PROP
    slot0 = iota((window, KDIM), 0)
    waiting = None
    for b, k in every:
        first = (len_ref[b] + acc_ref[b] - start) * heads
        base = jnp.clip((first // 16) * 16, 0, rows_block - window)
        base = pl.multiple_of(base, 16)
        placing = (row0 + (base - first) == wanted).astype(bf16)
        slot = slot0 + (base - first)
        written = jnp.logical_and(slot >= 0, slot < cols)
        fresh = head_rows(fresh_ref[b, :, k * columns : (k + 1) * columns], heads)
        placed = jnp.dot(placing, fresh, preferred_element_type=f32)
        load(b, k).wait()
        old = held[k][b, pl.ds(base, window), :].astype(f32)
        held[k][b, pl.ds(base, window), :] = jnp.where(written, placed, old).astype(bf16)
        if waiting is not None:
            store(*waiting).start()
        waiting = (b, k)
    store(*waiting).start()
    for b, k in every:
        store(b, k).wait()


def body(n, n_tp, tokens, norm_gain, w_query, w_key, w_value, lambdas, head_gain, w_out, cache_keys, cache_values, lengths, accepted, parents):
    sequences, positions, heads, _ = cache_keys.shape
    count, features = tokens.shape
    columns = heads * KDIM
    rows = 2 * heads * PROP
    block = positions * heads
    dma = pltpu.SemaphoreType.DMA
    flat = (sequences, block, KDIM)
    flat_keys, flat_values = cache_keys.reshape(flat), cache_values.reshape(flat)
    out_rows, out_columns = count // n_tp, w_out.shape[1]
    first_columns = columns + KDIM
    layer_out, fresh = pl.pallas_call(
        functools.partial(layer_kernel, n, n_tp),
        out_shape=(
            jax.ShapeDtypeStruct((out_rows, out_columns), bf16),
            jax.ShapeDtypeStruct((sequences, PROP, 2 * columns), bf16),
        ),
        in_specs=[VMEM, VMEM, ANY, ANY, ANY, SMEM, VMEM, ANY, ANY, ANY, SMEM, SMEM, VMEM],
        out_specs=(VMEM, VMEM),
        scratch_shapes=[
            pltpu.VMEM((3, features, columns), bf16),
            pltpu.VMEM(w_out.shape, bf16),
            pltpu.VMEM(flat, bf16),
            pltpu.VMEM(flat, bf16),
            pltpu.VMEM((sequences, PROP, 3 * columns + KDIM), f32),
            pltpu.VMEM((sequences, PROP, first_columns), bf16),
            pltpu.VMEM((sequences, PROP, columns), bf16),
            pltpu.VMEM((sequences, PROP, columns), bf16),
            pltpu.VMEM((n, PROP, first_columns), bf16),
            pltpu.VMEM((n, PROP, columns), bf16),
            pltpu.VMEM((n, PROP, columns), bf16),
            pltpu.VMEM((sequences, PROP, columns), bf16),
            pltpu.VMEM((PROP, KDIM), f32),
            pltpu.VMEM((heads, 8, block), f32),
            pltpu.VMEM((rows, block), f32),
            pltpu.VMEM((rows, block), f32),
            pltpu.VMEM((rows, block), bf16),
            pltpu.VMEM((rows, block), bf16),
            pltpu.VMEM((sequences, rows, KDIM), bf16),
            pltpu.VMEM((sequences, 8, KDIM), f32),
            pltpu.VMEM((n, rows, KDIM), bf16),
            pltpu.VMEM((n, 8, KDIM), f32),
            pltpu.VMEM((KDIM, KDIM), f32),
            pltpu.VMEM((sequences, PROP, columns), bf16),
            pltpu.VMEM((n_tp, out_rows, out_columns), bf16),
            pltpu.VMEM((n_tp, out_rows, out_columns), bf16),
            dma((4,)),
            dma((2, sequences)),
            dma((3, sequences)),
            dma((3, n)),
            dma((n,)),
            dma((sequences,)),
            dma((n,)),
            dma((sequences,)),
            dma((2, sequences)),
            dma((2, n)),
            dma((n,)),
            dma((sequences,)),
            dma((n_tp,)),
            dma((n_tp,)),
        ],
        compiler_params=pltpu.CompilerParams(collective_id=0, has_side_effects=True),
        name="layer",
    )(tokens, norm_gain.reshape(1, features), w_query, w_key, w_value, lambdas, head_gain.reshape(1, KDIM), w_out,
      flat_keys, flat_values, lengths, accepted, parents)

    keys_out, values_out = pl.pallas_call(
        functools.partial(place_kernel, heads),
        out_shape=(jax.ShapeDtypeStruct(flat, bf16), jax.ShapeDtypeStruct(flat, bf16)),
        in_specs=[SMEM, SMEM, VMEM, ANY, ANY],
        out_specs=(ANY, ANY),
        scratch_shapes=[
            pltpu.VMEM(flat, bf16),
            pltpu.VMEM(flat, bf16),
            dma((2, sequences)),
            dma((2, sequences)),
        ],
        name="place",
    )(lengths, accepted, fresh, flat_keys, flat_values)
    return (layer_out, keys_out.reshape(cache_keys.shape), values_out.reshape(cache_values.shape))


def solution(mesh):
    return jax.shard_map(
        functools.partial(body, mesh.shape["kv"], mesh.shape["tp"]),
        mesh=mesh,
        in_specs=(
            P(None, "kv"),
            P("kv"),
            P("kv", "tp"),
            P("kv", "tp"),
            P("kv", "tp"),
            P("tp"),
            P(),
            P("tp", "kv"),
            P(None, "kv", "tp", None),
            P(None, "kv", "tp", None),
            P(),
            P(),
            P(),
        ),
        out_specs=(P("tp", "kv"), P(None, "kv", "tp", None), P(None, "kv", "tp", None)),
        check_vma=False,
    )
```
